32 devices in a mesh: tp: 4 (over y, x), dp: 8 (over z, core).
Axes of the slice: x: 2, y: 2, z: 4, core: 2. Of those that a mesh axis runs over, the one named last changes fastest.
Arguments:
- tokens: bfloat16 [64, 4096], P('tp', 'dp'), may hold values from -12 to 12, as said below
- norm_gain: float32 [2, 4096], P(None, 'dp'), may hold values from 0.1 to 1.9
- w_input: bfloat16 [2, 4096, 2048], P(None, 'dp', 'tp'), may hold values from -0.09375 to 0.09375
- w_gate: bfloat16 [2, 4096, 2048], P(None, 'dp', 'tp'), may hold values from -0.09375 to 0.09375
- w_recur: bfloat16 [2, 16, 128, 128], P(None, 'tp'), may hold values from -0.5 to 0.5
- w_inject: bfloat16 [2, 16, 128, 128], P(None, 'tp'), may hold values from -0.5 to 0.5
- conv_weight: bfloat16 [2, 4, 2048], P(None, None, 'tp'), may hold values from -3 to 3
- decay_param: float32 [2, 2048], P(None, 'tp'), may hold values from -2 to 5
- w_output: bfloat16 [2, 2048, 4096], P(None, 'tp', 'dp'), may hold values from -0.125 to 0.125
- lengths: int32 [64], P('dp'), may hold values from 1 to 48, 512 in all
- conv_state: bfloat16 [2, 3, 64, 2048], P(None, None, 'dp', 'tp'), may hold values from -6 to 6
- rec_state: float32 [2, 64, 2048], P(None, 'dp', 'tp'), may hold values from -6 to 6
Outputs:
- mixed: bfloat16 [64, 4096], P('tp', 'dp')
- new_conv: bfloat16 [2, 3, 64, 2048], P(None, None, 'dp', 'tp')
- new_rec: float32 [2, 64, 2048], P(None, 'dp', 'tp')
The draws below stay inside these ranges and needn't reach their ends.
Inputs may be any that keep to these rules, and one draw needn't show every extreme that they name: `tokens`: activations; feature scales vary.
All inputs are finite; a program needn't handle non-finite values. No bound on the sum of `lengths` on one device may be relied on, other than what follows from the above.
Results may differ from the reference program's by a relative error of at most 0.02.
Values may be sent and summed in bfloat16 or wider, within the bound.
A program may use at most 64 MiB of HBM per device.

```python
import math
import jax
import jax.numpy as jnp
import numpy as np
from jax import lax

D = 4096
NB = 16
BLK = 128
CONV = 4
W = 2048
BATCH = 64


def draw_tokens(key, part):
    col_scale = jnp.exp(jnp.linspace(jnp.log(0.5), jnp.log(2.0), D)).astype(jnp.float32)
    values = jnp.clip(jax.random.normal(key, (BATCH, D), jnp.float32), -6.0, 6.0)
    return (values * col_scale).astype(jnp.bfloat16)


def block_levels(key, extent, shards, low, high):
    def one(dim, parts):
        heights = jax.random.uniform(jax.random.fold_in(jax.random.fold_in(key, 6), dim), (parts,), jnp.float32, low / len(shards), high / len(shards))
        return jnp.repeat(jnp.exp(heights), extent[dim] // parts).reshape((-1,) + (1,) * (len(extent) - dim - 1))

    gain = one(*shards[0])
    for cut in shards[1:]:
        gain = gain * one(*cut)
    return gain


def split_up(count, total, reach, slope):
    weights = [(1 << 20) // math.isqrt(grade ** slope) + 1 for grade in range(2, count + 1)]
    surplus, holding = total - reach - (count - 1), [1] * (count - 1)
    while surplus > 0:
        movable = [i for i in range(count - 1) if holding[i] < reach]
        pool, left = sum([weights[i] for i in movable]), surplus
        for i in movable:
            addition = min(reach - holding[i], max(1, left * weights[i] // pool), surplus)
            holding[i] = holding[i] + addition
            surplus = surplus - addition
    return np.array([reach] + holding)


def uneven_parts(own_key, count, total, reach, slope):
    if count == 2:
        one = jax.random.randint(own_key, (), max(1, total - reach), min(reach, total - 1) + 1)
        return jnp.stack([one, total - one])
    sizes = jnp.asarray(split_up(count, total, reach, slope), jnp.int32)
    couples = (count - 1) // 2
    source_of, receiver = sizes[1:1 + 2 * couples:2], sizes[2:2 + 2 * couples:2]
    slack = jnp.minimum(source_of - 1, reach - receiver)
    shifted = jax.random.randint(jax.random.fold_in(own_key, 1), (couples,), 0, 1 << 20) % (slack + 1)
    sizes = sizes.at[1:1 + 2 * couples:2].set(source_of - shifted).at[2:2 + 2 * couples:2].set(receiver + shifted)
    return sizes[jax.random.permutation(jax.random.fold_in(own_key, 2), count)]


def bell_draw(key, dims, deviation, most, cuts=(), dtype=jnp.bfloat16):
    gain = block_levels(key, dims, cuts, -0.22, 0.18) if cuts else 1.0
    array = jax.random.normal(key, dims, jnp.float32) * deviation * gain
    return jnp.minimum(jnp.maximum(array, -most), most).astype(dtype)


def setup_inputs(seed: int = 0) -> dict:
    streams_of = jax.random.split(jax.random.key(seed), 13)
    return {
        "tokens": draw_tokens(jax.random.fold_in(streams_of[12], 71), 0),
        "norm_gain": jnp.clip(1.0 + 0.18 * jax.random.normal(streams_of[1], (2, D), jnp.float32), 0.1, 1.9),
        "w_input": bell_draw(streams_of[2], (2, D, W), D ** -0.5, 0.09375, ((1, 8), (2, 4))),
        "w_gate": bell_draw(streams_of[3], (2, D, W), D ** -0.5, 0.09375, ((1, 8), (2, 4))),
        "w_recur": bell_draw(streams_of[4], (2, NB, BLK, BLK), BLK ** -0.5, 0.5, ((1, 4),)),
        "w_inject": bell_draw(streams_of[5], (2, NB, BLK, BLK), BLK ** -0.5, 0.5, ((1, 4),)),
        "conv_weight": bell_draw(streams_of[6], (2, CONV, W), CONV ** -0.5, 3.0, ((2, 4),)),
        "decay_param": jnp.clip(-2.0 + 7.0 * jax.random.uniform(streams_of[7], (2, W), jnp.float32) ** block_levels(streams_of[7], (2, W), ((1, 4),), -0.2, 0.2), -2.0, 5.0),
        "w_output": bell_draw(streams_of[8], (2, W, D), W ** -0.5, 0.125, ((1, 4), (2, 8))),
        "lengths": uneven_parts(streams_of[9], BATCH, 8 * BATCH, 48, 2).astype(jnp.int32),
        "conv_state": bell_draw(streams_of[10], (2, CONV - 1, BATCH, W), 1.0, 6.0, ((2, 8), (3, 4))),
        "rec_state": bell_draw(streams_of[11], (2, BATCH, W), 1.0, 6.0, ((1, 8), (2, 4)), jnp.float32),
    }


EPS = 1e-06

def reference(tokens, norm_gain, w_input, w_gate, w_recur, w_inject, conv_weight, decay_param, w_output, lengths, conv_state, rec_state):
    current = tokens
    live_len = lengths[:, None]
    conv_list = []
    rec_list = []
    for layer_idx in range(2):
        widened = current.astype(jnp.float32)
        rscale = lax.rsqrt(lax.optimization_barrier(jnp.mean(widened * widened, axis=1, keepdims=True)) + EPS)
        scaled = (widened * norm_gain[layer_idx]).astype(jnp.bfloat16)
        value_in = jnp.dot(scaled, w_input[layer_idx], preferred_element_type=jnp.float32) * rscale
        gate_in = jnp.dot(scaled, w_gate[layer_idx], preferred_element_type=jnp.float32) * rscale
        conv_taps = conv_weight[layer_idx].astype(jnp.float32)
        old_taps = conv_state[layer_idx]
        tap_count = old_taps.shape[0]
        conv_out = conv_taps[tap_count] * value_in
        for back in range(1, tap_count + 1):
            conv_out = conv_out + conv_taps[tap_count - back] * jnp.where(back < live_len, old_taps[tap_count - back].astype(jnp.float32), jnp.float32(0.0))
        conv_low = conv_out.astype(jnp.bfloat16).reshape(BATCH, NB, BLK).astype(jnp.float32)
        rec_gate = jax.nn.sigmoid(jnp.einsum('bnc,ncd->bnd', conv_low, w_recur[layer_idx].astype(jnp.float32)).reshape(BATCH, W))
        inp_gate = jax.nn.sigmoid(jnp.einsum('bnc,ncd->bnd', conv_low, w_inject[layer_idx].astype(jnp.float32)).reshape(BATCH, W))
        log_decay = -8.0 * rec_gate * jax.nn.softplus(-decay_param[layer_idx])
        previous = jnp.where(live_len > 1, rec_state[layer_idx], jnp.float32(0.0))
        hidden = jnp.exp(log_decay) * previous + jnp.sqrt(-jnp.expm1(2.0 * log_decay)) * (inp_gate * conv_out)
        readout = (hidden * jax.nn.gelu(gate_in)).astype(jnp.bfloat16)
        current = (widened + jnp.dot(readout, w_output[layer_idx], preferred_element_type=jnp.float32)).astype(jnp.bfloat16)
        conv_list.append(jnp.concatenate([old_taps[1:], value_in.astype(jnp.bfloat16)[None]], axis=0))
        rec_list.append(hidden)
    return (current, jnp.stack(conv_list), jnp.stack(rec_list))
```

```python
import functools

import jax
import jax.numpy as jnp
from jax import lax
from jax.experimental import pallas as pl
from jax.experimental.pallas import tpu as pltpu
from jax.sharding import PartitionSpec as P

EPS = 1e-06
MESH = pl.DeviceIdType.MESH
LANES = 128


def shift_order(count):
    return sorted(range(1, count), key=lambda s: (-min(s, count - s), s))


def kernel(
    n_tp,
    n_dp,
    tokens,
    norm_gain,
    w_input,
    w_gate,
    w_recur,
    w_inject,
    conv_weight,
    decay_param,
    w_output,
    lengths,
    conv_state,
    rec_state,
    mixed,
    new_conv,
    new_rec,
    gain_v,
    win_v,
    wgate_v,
    wrec_v,
    winj_v,
    cw_v,
    decay_v,
    wout_v,
    len_s,
    cs_v,
    rs_v,
    x_all,
    x_keep,
    sq_out,
    sq_in,
    val_out,
    val_in,
    gate_out,
    gate_in_buf,
    read_all,
    part_all,
    last_out,
    last_in,
    load_sem,
    tok_send,
    tok_recv,
    sq_send,
    sq_recv,
    val_send,
    val_recv,
    gate_send,
    gate_recv,
    read_send,
    read_recv,
    part_send,
    part_recv,
):
    me_tp = lax.axis_index("tp")
    me_dp = lax.axis_index("dp")
    layers = w_input.shape[0]
    rows, width = tokens.shape
    state_rows = lengths.shape[0]
    chans = w_input.shape[2]
    taps = conv_state.shape[1]
    blocks, blk = w_recur.shape[1], w_recur.shape[2]
    all_rows = rows * n_tp
    model = width * n_dp

    loads = {}

    def load(name, src, dst, idx):
        copy = pltpu.make_async_copy(src, dst, load_sem.at[idx])
        copy.start()
        loads[name] = copy

    load("tokens", tokens, x_all.at[me_tp], 0)
    load("gain", norm_gain, gain_v, 1)
    load("win", w_input, win_v, 2)
    load("wgate", w_gate, wgate_v, 3)
    load("cw", conv_weight, cw_v, 4)
    load("decay", decay_param, decay_v, 5)
    load("len", lengths, len_s, 6)
    load("cs", conv_state, cs_v, 7)
    load("rs", rec_state, rs_v, 8)
    load("wrec", w_recur, wrec_v, 9)
    load("winj", w_inject, winj_v, 10)
    load("wout", w_output, wout_v, 11)

    barrier = pltpu.get_barrier_semaphore()
    for s in range(1, n_tp):
        pl.semaphore_signal(
            barrier, inc=1, device_id={"tp": lax.rem(me_tp + s, n_tp)}, device_id_type=MESH
        )
    for s in range(1, n_dp):
        pl.semaphore_signal(
            barrier, inc=1, device_id={"dp": lax.rem(me_dp + s, n_dp)}, device_id_type=MESH
        )
    loads["tokens"].wait()
    pl.semaphore_wait(barrier, n_tp + n_dp - 2)

    sent = []

    def send(src, dst, send_sem, recv_sem, axis, target):
        copy = pltpu.make_async_remote_copy(
            src_ref=src,
            dst_ref=dst,
            send_sem=send_sem,
            recv_sem=recv_sem,
            device_id={axis: target},
            device_id_type=MESH,
        )
        copy.start()
        sent.append(copy)
        return copy

    def gather(buf, send_sems, recv_sems, axis, me, count):
        copies = []
        for s in shift_order(count):
            copies.append(
                send(
                    buf.at[me],
                    buf.at[me],
                    send_sems.at[s],
                    recv_sems.at[s],
                    axis,
                    lax.rem(me + s, count),
                )
            )
        return copies

    def scatter(out, into, send_sems, recv_sems, axis, me, count):
        copies = []
        for s in shift_order(count):
            target = lax.rem(me + s, count)
            copies.append(
                send(out.at[target], into.at[s], send_sems.at[s], recv_sems.at[s], axis, target)
            )
        return copies

    def arrive(copies):
        for copy in copies:
            copy.wait_recv()

    tok = gather(x_all, tok_send, tok_recv, "tp", me_tp, n_tp)

    loads["len"].wait()
    row_id = lax.broadcasted_iota(jnp.int32, (state_rows, chans), 0)
    live_len = jnp.zeros((state_rows, chans), jnp.int32)
    for r in range(state_rows):
        live_len = jnp.where(row_id == r, len_s[r], live_len)
    loads["decay"].wait()
    neg = -decay_v[...]
    rate = -8.0 * (jnp.maximum(neg, 0.0) + jnp.log1p(jnp.exp(-jnp.abs(neg))))
    loads["gain"].wait()
    gains = gain_v[...]

    arrive(tok)
    current = x_all[...].astype(jnp.float32).reshape(all_rows, width)

    for l in range(layers):
        squares = None
        for c in range(0, width, LANES):
            piece = current[:, c : c + LANES]
            squares = piece * piece if squares is None else squares + piece * piece
        sq_out[l] = squares.reshape(n_dp, state_rows, LANES)
        sq_copies = scatter(
            sq_out.at[l], sq_in.at[l], sq_send.at[l], sq_recv.at[l], "dp", me_dp, n_dp
        )
        scaled = (current * gains[l : l + 1]).astype(jnp.bfloat16)
        if l == 0:
            loads["win"].wait()
        part = jnp.dot(scaled, win_v[l], preferred_element_type=jnp.float32)
        val_out[l] = part.reshape(n_dp, state_rows, chans).astype(jnp.bfloat16)
        val_copies = scatter(
            val_out.at[l], val_in.at[l], val_send.at[l], val_recv.at[l], "dp", me_dp, n_dp
        )
        if l == 0:
            loads["wgate"].wait()
        part = jnp.dot(scaled, wgate_v[l], preferred_element_type=jnp.float32)
        gate_out[l] = part.reshape(n_dp, state_rows, chans).astype(jnp.bfloat16)
        gate_copies = scatter(
            gate_out.at[l], gate_in_buf.at[l], gate_send.at[l], gate_recv.at[l], "dp", me_dp, n_dp
        )

        if l == 0:
            for name in ("cw", "cs", "rs", "wrec", "winj"):
                loads[name].wait()
        conv_taps = cw_v[l].astype(jnp.float32)
        old = [cs_v[l, t].astype(jnp.float32) for t in range(taps)]
        history = jnp.zeros((state_rows, chans), jnp.float32)
        for back in range(1, taps + 1):
            history = history + conv_taps[taps - back : taps - back + 1] * jnp.where(
                back < live_len, old[taps - back], 0.0
            )
        previous = jnp.where(live_len > 1, rs_v[l], 0.0)
        for t in range(1, taps):
            new_conv[l, t - 1] = cs_v[l, t]

        arrive(sq_copies)
        total = sq_out[l, me_dp]
        for s in range(1, n_dp):
            total = total + sq_in[l, s]
        scale = lax.rsqrt(jnp.sum(total, axis=1, keepdims=True) / model + EPS)
        arrive(val_copies)
        value = val_out[l, me_dp].astype(jnp.float32)
        for s in range(1, n_dp):
            value = value + val_in[l, s].astype(jnp.float32)
        value = value * scale
        new_conv[l, taps - 1] = value.astype(jnp.bfloat16)
        conv_out = conv_taps[taps : taps + 1] * value + history
        conv_low = conv_out.astype(jnp.bfloat16)
        rec_parts = []
        inj_parts = []
        for b in range(blocks):
            piece = conv_low[:, b * blk : (b + 1) * blk]
            rec_parts.append(jnp.dot(piece, wrec_v[l, b], preferred_element_type=jnp.float32))
            inj_parts.append(jnp.dot(piece, winj_v[l, b], preferred_element_type=jnp.float32))
        rec_gate = jax.nn.sigmoid(jnp.concatenate(rec_parts, axis=1))
        inp_gate = jax.nn.sigmoid(jnp.concatenate(inj_parts, axis=1))
        log_decay = rate[l : l + 1] * rec_gate
        half = jnp.tanh(log_decay)
        hidden = jnp.exp(log_decay) * previous + jnp.sqrt(-2.0 * half / (1.0 - half)) * (
            inp_gate * conv_out
        )
        new_rec[l] = hidden
        arrive(gate_copies)
        gate = gate_out[l, me_dp].astype(jnp.float32)
        for s in range(1, n_dp):
            gate = gate + gate_in_buf[l, s].astype(jnp.float32)
        gate = gate * scale
        read_all[l, me_dp] = (hidden * jax.nn.gelu(gate)).astype(jnp.bfloat16)
        arrive(
            gather(read_all.at[l], read_send.at[l], read_recv.at[l], "dp", me_dp, n_dp)
        )
        reads = read_all[l].astype(jnp.float32).reshape(all_rows, chans).astype(jnp.bfloat16)
        if l == 0:
            loads["wout"].wait()
        branch = jnp.dot(reads, wout_v[l], preferred_element_type=jnp.float32)
        if l < layers - 1:
            part_all[l, me_tp] = branch.astype(jnp.bfloat16)
            arrive(
                gather(part_all.at[l], part_send.at[l], part_recv.at[l], "tp", me_tp, n_tp)
            )
            for j in range(n_tp):
                current = current + part_all[l, j].astype(jnp.float32)
            current = current.astype(jnp.bfloat16)
            x_keep[...] = current.reshape(n_tp, rows, width)
            current = current.astype(jnp.float32)
        else:
            last_out[...] = branch.reshape(n_tp, rows, width).astype(jnp.bfloat16)
            arrive(
                scatter(last_out, last_in, part_send.at[l], part_recv.at[l], "tp", me_tp, n_tp)
            )
            final = (x_keep if l else x_all)[me_tp].astype(jnp.float32) + last_out[me_tp].astype(jnp.float32)
            for s in range(1, n_tp):
                final = final + last_in[s].astype(jnp.float32)
            mixed[...] = final.astype(jnp.bfloat16)
    for copy in sent:
        copy.wait_send()


def body(n_tp, n_dp, *args):
    (tokens, norm_gain, w_input, w_gate, w_recur, w_inject, conv_weight, decay_param, w_output,
     lengths, conv_state, rec_state) = args
    layers = w_input.shape[0]
    rows, width = tokens.shape
    state_rows = lengths.shape[0]
    chans = w_input.shape[2]
    all_rows = rows * n_tp
    bf16, f32 = jnp.bfloat16, jnp.float32
    like = lambda a: pltpu.VMEM(a.shape, a.dtype)
    dma = pltpu.SemaphoreType.DMA
    vmem = pl.BlockSpec(memory_space=pltpu.VMEM)
    return pl.pallas_call(
        functools.partial(kernel, n_tp, n_dp),
        out_shape=(
            jax.ShapeDtypeStruct(tokens.shape, bf16),
            jax.ShapeDtypeStruct(conv_state.shape, bf16),
            jax.ShapeDtypeStruct(rec_state.shape, f32),
        ),
        in_specs=[pl.BlockSpec(memory_space=pl.ANY)] * len(args),
        out_specs=(vmem, vmem, vmem),
        scratch_shapes=[
            like(norm_gain),
            like(w_input),
            like(w_gate),
            like(w_recur),
            like(w_inject),
            like(conv_weight),
            like(decay_param),
            like(w_output),
            pltpu.SMEM(lengths.shape, lengths.dtype),
            like(conv_state),
            like(rec_state),
            pltpu.VMEM((n_tp, rows, width), bf16),
            pltpu.VMEM((n_tp, rows, width), bf16),
            pltpu.VMEM((layers, n_dp, state_rows, LANES), f32),
            pltpu.VMEM((layers, n_dp, state_rows, LANES), f32),
            pltpu.VMEM((layers, n_dp, state_rows, chans), bf16),
            pltpu.VMEM((layers, n_dp, state_rows, chans), bf16),
            pltpu.VMEM((layers, n_dp, state_rows, chans), bf16),
            pltpu.VMEM((layers, n_dp, state_rows, chans), bf16),
            pltpu.VMEM((layers, n_dp, state_rows, chans), bf16),
            pltpu.VMEM((layers, n_tp, all_rows, width), bf16),
            pltpu.VMEM((n_tp, rows, width), bf16),
            pltpu.VMEM((n_tp, rows, width), bf16),
            dma((12,)),
            dma((n_tp,)),
            dma((n_tp,)),
            dma((layers, n_dp)),
            dma((layers, n_dp)),
            dma((layers, n_dp)),
            dma((layers, n_dp)),
            dma((layers, n_dp)),
            dma((layers, n_dp)),
            dma((layers, n_dp)),
            dma((layers, n_dp)),
            dma((layers, n_tp)),
            dma((layers, n_tp)),
        ],
        compiler_params=pltpu.CompilerParams(collective_id=0, has_side_effects=True),
    )(*args)


def solution(mesh):
    n_tp, n_dp = mesh.shape["tp"], mesh.shape["dp"]
    placed = (
        P("tp", "dp"),
        P(None, "dp"),
        P(None, "dp", "tp"),
        P(None, "dp", "tp"),
        P(None, "tp", None, None),
        P(None, "tp", None, None),
        P(None, None, "tp"),
        P(None, "tp"),
        P(None, "tp", "dp"),
        P("dp"),
        P(None, None, "dp", "tp"),
        P(None, "dp", "tp"),
    )
    return jax.shard_map(
        functools.partial(body, n_tp, n_dp),
        mesh=mesh,
        in_specs=placed,
        out_specs=(P("tp", "dp"), P(None, None, "dp", "tp"), P(None, "dp", "tp")),
        check_vma=False,
    )
```

```python
import functools

import jax
import jax.numpy as jnp
from jax import lax
from jax.experimental import pallas as pl
from jax.experimental.pallas import tpu as pltpu
from jax.sharding import PartitionSpec as P

EPS = 1e-06
MESH = pl.DeviceIdType.MESH
LANES = 128


def order_of(count):
    return sorted(range(1, count), reverse=True)


def partner(me, step, count):
    if count & (count - 1):
        return lax.rem(count + step - me, count)
    other, bit = me, 1
    while bit < count:
        if step & bit:
            other = other + bit - 2 * bit * lax.rem(me // bit, 2)
        bit *= 2
    return other


def kernel(
    n_tp,
    n_dp,
    tokens,
    norm_gain,
    w_input,
    w_gate,
    w_recur,
    w_inject,
    conv_weight,
    decay_param,
    w_output,
    lengths,
    conv_state,
    rec_state,
    mixed,
    new_conv,
    new_rec,
    gain_v,
    win_v,
    wgate_v,
    wrec_v,
    winj_v,
    cw_v,
    decay_v,
    wout_v,
    len_s,
    cs_v,
    rs_v,
    x_all,
    x_keep,
    sq_out,
    sq_in,
    val_out,
    val_in,
    gate_out,
    gate_in_buf,
    read_all,
    part_all,
    last_out,
    last_in,
    load_sem,
    tok_send,
    tok_recv,
    sq_send,
    sq_recv,
    val_send,
    val_recv,
    gate_send,
    gate_recv,
    read_send,
    read_recv,
    part_send,
    part_recv,
):
    me_tp = lax.axis_index("tp")
    me_dp = lax.axis_index("dp")
    layers = w_input.shape[0]
    rows, width = tokens.shape
    state_rows = lengths.shape[0]
    chans = w_input.shape[2]
    taps = conv_state.shape[1]
    blocks, blk = w_recur.shape[1], w_recur.shape[2]
    all_rows = rows * n_tp
    model = width * n_dp

    loads = {}

    def load(name, src, dst, idx):
        copy = pltpu.make_async_copy(src, dst, load_sem.at[idx])
        copy.start()
        loads[name] = copy

    load("tokens", tokens, x_all.at[me_tp], 0)
    barrier = pltpu.get_barrier_semaphore()
    for s in range(1, n_tp):
        pl.semaphore_signal(
            barrier, inc=1, device_id={"tp": lax.rem(me_tp + s, n_tp)}, device_id_type=MESH
        )
    for s in range(1, n_dp):
        pl.semaphore_signal(
            barrier, inc=1, device_id={"dp": lax.rem(me_dp + s, n_dp)}, device_id_type=MESH
        )
    load("gain", norm_gain, gain_v, 1)
    load("win", w_input, win_v, 2)
    load("wgate", w_gate, wgate_v, 3)
    load("cw", conv_weight, cw_v, 4)
    load("decay", decay_param, decay_v, 5)
    load("len", lengths, len_s, 6)
    load("cs", conv_state, cs_v, 7)
    load("rs", rec_state, rs_v, 8)
    load("wrec", w_recur, wrec_v, 9)
    load("winj", w_inject, winj_v, 10)
    load("wout", w_output, wout_v, 11)

    loads["tokens"].wait()
    pl.semaphore_wait(barrier, n_tp + n_dp - 2)

    sent = []

    def send(src, dst, send_sem, recv_sem, axis, target):
        copy = pltpu.make_async_remote_copy(
            src_ref=src,
            dst_ref=dst,
            send_sem=send_sem,
            recv_sem=recv_sem,
            device_id={axis: target},
            device_id_type=MESH,
        )
        copy.start()
        sent.append(copy)
        return copy

    def gather(buf, send_sems, recv_sems, axis, me, count):
        copies = []
        for s in order_of(count):
            copies.append(
                send(
                    buf.at[me],
                    buf.at[me],
                    send_sems.at[s],
                    recv_sems.at[s],
                    axis,
                    partner(me, s, count),
                )
            )
        return copies

    def scatter(out, into, send_sems, recv_sems, axis, me, count):
        copies = []
        for s in order_of(count):
            target = partner(me, s, count)
            copies.append(
                send(out.at[target], into.at[s], send_sems.at[s], recv_sems.at[s], axis, target)
            )
        return copies

    def arrive(copies):
        for copy in copies:
            copy.wait_recv()

    tok = gather(x_all, tok_send, tok_recv, "tp", me_tp, n_tp)

    loads["len"].wait()
    row_id = lax.broadcasted_iota(jnp.int32, (state_rows, chans), 0)
    live_len = jnp.zeros((state_rows, chans), jnp.int32)
    for r in range(state_rows):
        live_len = jnp.where(row_id == r, len_s[r], live_len)
    loads["decay"].wait()
    neg = -decay_v[...]
    rate = -8.0 * (jnp.maximum(neg, 0.0) + jnp.log1p(jnp.exp(-jnp.abs(neg))))
    loads["gain"].wait()
    gains = gain_v[...]

    arrive(tok)
    current = x_all[...].astype(jnp.float32).reshape(all_rows, width)

    for l in range(layers):
        squares = None
        for c in range(0, width, LANES):
            piece = current[:, c : c + LANES]
            squares = piece * piece if squares is None else squares + piece * piece
        sq_out[l] = squares.reshape(n_dp, state_rows, LANES)
        sq_copies = scatter(
            sq_out.at[l], sq_in.at[l], sq_send.at[l], sq_recv.at[l], "dp", me_dp, n_dp
        )
        scaled = (current * gains[l : l + 1]).astype(jnp.bfloat16)
        if l == 0:
            loads["win"].wait()
        part = jnp.dot(scaled, win_v[l], preferred_element_type=jnp.float32)
        val_out[l] = part.reshape(n_dp, state_rows, chans).astype(jnp.bfloat16)
        val_copies = scatter(
            val_out.at[l], val_in.at[l], val_send.at[l], val_recv.at[l], "dp", me_dp, n_dp
        )
        if l == 0:
            loads["wgate"].wait()
        part = jnp.dot(scaled, wgate_v[l], preferred_element_type=jnp.float32)
        gate_out[l] = part.reshape(n_dp, state_rows, chans).astype(jnp.bfloat16)
        gate_copies = scatter(
            gate_out.at[l], gate_in_buf.at[l], gate_send.at[l], gate_recv.at[l], "dp", me_dp, n_dp
        )

        if l == 0:
            for name in ("cw", "cs", "rs", "wrec", "winj"):
                loads[name].wait()
        conv_taps = cw_v[l].astype(jnp.float32)
        old = [cs_v[l, t].astype(jnp.float32) for t in range(taps)]
        history = jnp.zeros((state_rows, chans), jnp.float32)
        for back in range(1, taps + 1):
            history = history + conv_taps[taps - back : taps - back + 1] * jnp.where(
                back < live_len, old[taps - back], 0.0
            )
        previous = jnp.where(live_len > 1, rs_v[l], 0.0)
        for t in range(1, taps):
            new_conv[l, t - 1] = cs_v[l, t]

        arrive(sq_copies)
        total = sq_out[l, me_dp]
        for s in range(1, n_dp):
            total = total + sq_in[l, s]
        scale = lax.rsqrt(jnp.sum(total, axis=1, keepdims=True) / model + EPS)
        arrive(val_copies)
        value = val_out[l, me_dp].astype(jnp.float32)
        for s in range(1, n_dp):
            value = value + val_in[l, s].astype(jnp.float32)
        value = value * scale
        new_conv[l, taps - 1] = value.astype(jnp.bfloat16)
        conv_out = conv_taps[taps : taps + 1] * value + history
        conv_low = conv_out.astype(jnp.bfloat16)
        rec_parts = []
        inj_parts = []
        for b in range(blocks):
            piece = conv_low[:, b * blk : (b + 1) * blk]
            rec_parts.append(jnp.dot(piece, wrec_v[l, b], preferred_element_type=jnp.float32))
            inj_parts.append(jnp.dot(piece, winj_v[l, b], preferred_element_type=jnp.float32))
        rec_gate = jax.nn.sigmoid(jnp.concatenate(rec_parts, axis=1))
        inp_gate = jax.nn.sigmoid(jnp.concatenate(inj_parts, axis=1))
        log_decay = rate[l : l + 1] * rec_gate
        half = jnp.tanh(log_decay)
        hidden = jnp.exp(log_decay) * previous + jnp.sqrt(-2.0 * half / (1.0 - half)) * (
            inp_gate * conv_out
        )
        new_rec[l] = hidden
        arrive(gate_copies)
        gate = gate_out[l, me_dp].astype(jnp.float32)
        for s in range(1, n_dp):
            gate = gate + gate_in_buf[l, s].astype(jnp.float32)
        gate = gate * scale
        read_all[l, me_dp] = (hidden * jax.nn.gelu(gate)).astype(jnp.bfloat16)
        arrive(
            gather(read_all.at[l], read_send.at[l], read_recv.at[l], "dp", me_dp, n_dp)
        )
        reads = read_all[l].astype(jnp.float32).reshape(all_rows, chans).astype(jnp.bfloat16)
        if l == 0:
            loads["wout"].wait()
        branch = jnp.dot(reads, wout_v[l], preferred_element_type=jnp.float32)
        if l < layers - 1:
            part_all[l, me_tp] = branch.astype(jnp.bfloat16)
            arrive(
                gather(part_all.at[l], part_send.at[l], part_recv.at[l], "tp", me_tp, n_tp)
            )
            for j in range(n_tp):
                current = current + part_all[l, j].astype(jnp.float32)
            current = current.astype(jnp.bfloat16)
            x_keep[...] = current.reshape(n_tp, rows, width)
            current = current.astype(jnp.float32)
        else:
            last_out[...] = branch.reshape(n_tp, rows, width).astype(jnp.bfloat16)
            arrive(
                scatter(last_out, last_in, part_send.at[l], part_recv.at[l], "tp", me_tp, n_tp)
            )
            final = (x_keep if l else x_all)[me_tp].astype(jnp.float32) + last_out[me_tp].astype(jnp.float32)
            for s in range(1, n_tp):
                final = final + last_in[s].astype(jnp.float32)
            mixed[...] = final.astype(jnp.bfloat16)
    for copy in sent:
        copy.wait_send()


def flush(*refs):
    count = len(refs) // 2
    sems = refs[-1]
    copies = [
        pltpu.make_async_copy(src, dst, sems.at[i])
        for i, (src, dst) in enumerate(zip(refs[:count], refs[count : 2 * count]))
    ]
    for copy in copies:
        copy.start()
    for copy in copies:
        copy.wait()


def body(n_tp, n_dp, *args):
    (tokens, norm_gain, w_input, w_gate, w_recur, w_inject, conv_weight, decay_param, w_output,
     lengths, conv_state, rec_state) = args
    layers = w_input.shape[0]
    rows, width = tokens.shape
    state_rows = lengths.shape[0]
    chans = w_input.shape[2]
    all_rows = rows * n_tp
    bf16, f32 = jnp.bfloat16, jnp.float32
    like = lambda a: pltpu.VMEM(a.shape, a.dtype)
    dma = pltpu.SemaphoreType.DMA
    vmem = pl.BlockSpec(memory_space=pltpu.VMEM)
    shapes = ((tokens.shape, bf16), (conv_state.shape, bf16), (rec_state.shape, f32))
    held = pl.pallas_call(
        functools.partial(kernel, n_tp, n_dp),
        out_shape=tuple(pltpu.VMEM(*each) for each in shapes),
        in_specs=[pl.BlockSpec(memory_space=pl.ANY)] * len(args),
        out_specs=(vmem, vmem, vmem),
        scratch_shapes=[
            like(norm_gain),
            like(w_input),
            like(w_gate),
            like(w_recur),
            like(w_inject),
            like(conv_weight),
            like(decay_param),
            like(w_output),
            pltpu.SMEM(lengths.shape, lengths.dtype),
            like(conv_state),
            like(rec_state),
            pltpu.VMEM((n_tp, rows, width), bf16),
            pltpu.VMEM((n_tp, rows, width), bf16),
            pltpu.VMEM((layers, n_dp, state_rows, LANES), f32),
            pltpu.VMEM((layers, n_dp, state_rows, LANES), f32),
            pltpu.VMEM((layers, n_dp, state_rows, chans), bf16),
            pltpu.VMEM((layers, n_dp, state_rows, chans), bf16),
            pltpu.VMEM((layers, n_dp, state_rows, chans), bf16),
            pltpu.VMEM((layers, n_dp, state_rows, chans), bf16),
            pltpu.VMEM((layers, n_dp, state_rows, chans), bf16),
            pltpu.VMEM((layers, n_tp, all_rows, width), bf16),
            pltpu.VMEM((n_tp, rows, width), bf16),
            pltpu.VMEM((n_tp, rows, width), bf16),
            dma((12,)),
            dma((n_tp,)),
            dma((n_tp,)),
            dma((layers, n_dp)),
            dma((layers, n_dp)),
            dma((layers, n_dp)),
            dma((layers, n_dp)),
            dma((layers, n_dp)),
            dma((layers, n_dp)),
            dma((layers, n_dp)),
            dma((layers, n_dp)),
            dma((layers, n_tp)),
            dma((layers, n_tp)),
        ],
        compiler_params=pltpu.CompilerParams(collective_id=0, has_side_effects=True),
    )(*args)
    return pl.pallas_call(
        flush,
        out_shape=tuple(jax.ShapeDtypeStruct(*each) for each in shapes),
        in_specs=[vmem] * len(shapes),
        out_specs=tuple(pl.BlockSpec(memory_space=pl.ANY) for _ in shapes),
        scratch_shapes=[dma((len(shapes),))],
    )(*[pltpu.with_memory_space_constraint(each, pltpu.VMEM) for each in held])


def solution(mesh):
    n_tp, n_dp = mesh.shape["tp"], mesh.shape["dp"]
    placed = (
        P("tp", "dp"),
        P(None, "dp"),
        P(None, "dp", "tp"),
        P(None, "dp", "tp"),
        P(None, "tp", None, None),
        P(None, "tp", None, None),
        P(None, None, "tp"),
        P(None, "tp"),
        P(None, "tp", "dp"),
        P("dp"),
        P(None, None, "dp", "tp"),
        P(None, "dp", "tp"),
    )
    return jax.shard_map(
        functools.partial(body, n_tp, n_dp),
        mesh=mesh,
        in_specs=placed,
        out_specs=(P("tp", "dp"), P(None, None, "dp", "tp"), P(None, "dp", "tp")),
        check_vma=False,
    )
```

```python
import functools

import jax
import jax.numpy as jnp
from jax import lax
from jax.experimental import pallas as pl
from jax.experimental.pallas import tpu as pltpu
from jax.sharding import PartitionSpec as P

EPS = 1e-06
MESH = pl.DeviceIdType.MESH
LANES = 128


def order_of(count):
    return sorted(range(1, count), reverse=True)


def partner(me, step, count):
    if count & (count - 1):
        return lax.rem(count + step - me, count)
    other, bit = me, 1
    while bit < count:
        if step & bit:
            other = other + bit - 2 * bit * lax.rem(me // bit, 2)
        bit *= 2
    return other


def kernel(
    n_tp,
    n_dp,
    tokens,
    norm_gain,
    w_input,
    w_gate,
    w_recur,
    w_inject,
    conv_weight,
    decay_param,
    w_output,
    lengths,
    conv_state,
    rec_state,
    mixed,
    new_conv,
    new_rec,
    gain_v,
    win_v,
    wgate_v,
    wrec_v,
    winj_v,
    cw_v,
    decay_v,
    wout_v,
    len_s,
    cs_v,
    rs_v,
    x_all,
    x_keep,
    sq_out,
    sq_in,
    val_out,
    val_in,
    gate_out,
    gate_in_buf,
    read_all,
    part_all,
    last_out,
    last_in,
    load_sem,
    tok_send,
    tok_recv,
    sq_send,
    sq_recv,
    val_send,
    val_recv,
    gate_send,
    gate_recv,
    read_send,
    read_recv,
    part_send,
    part_recv,
    last_send,
    last_recv,
):
    me_tp = lax.axis_index("tp")
    me_dp = lax.axis_index("dp")
    layers = w_input.shape[0]
    rows, width = tokens.shape
    state_rows = lengths.shape[0]
    chans = w_input.shape[2]
    taps = conv_state.shape[1]
    blocks, blk = w_recur.shape[1], w_recur.shape[2]
    all_rows = rows * n_tp
    model = width * n_dp

    loads = {}

    def load(name, src, dst, idx):
        copy = pltpu.make_async_copy(src, dst, load_sem.at[idx])
        copy.start()
        loads[name] = copy

    load("tokens", tokens, x_all.at[me_tp], 0)
    barrier = pltpu.get_barrier_semaphore()
    for s in range(1, n_tp):
        pl.semaphore_signal(
            barrier, inc=1, device_id={"tp": lax.rem(me_tp + s, n_tp)}, device_id_type=MESH
        )
    for s in range(1, n_dp):
        pl.semaphore_signal(
            barrier, inc=1, device_id={"dp": lax.rem(me_dp + s, n_dp)}, device_id_type=MESH
        )
    load("gain", norm_gain, gain_v, 1)
    load("win", w_input, win_v, 2)
    load("wgate", w_gate, wgate_v, 3)
    load("cw", conv_weight, cw_v, 4)
    load("decay", decay_param, decay_v, 5)
    load("len", lengths, len_s, 6)
    load("cs", conv_state, cs_v, 7)
    load("rs", rec_state, rs_v, 8)
    load("wrec", w_recur, wrec_v, 9)
    load("winj", w_inject, winj_v, 10)
    load("wout", w_output, wout_v, 11)

    loads["tokens"].wait()
    pl.semaphore_wait(barrier, n_tp + n_dp - 2)

    sent = []

    def send(src, dst, send_sem, recv_sem, axis, target):
        copy = pltpu.make_async_remote_copy(
            src_ref=src,
            dst_ref=dst,
            send_sem=send_sem,
            recv_sem=recv_sem,
            device_id={axis: target},
            device_id_type=MESH,
        )
        copy.start()
        sent.append(copy)
        return copy

    def gather(buf, send_sems, recv_sems, axis, me, count):
        copies = []
        for s in order_of(count):
            copies.append(
                send(
                    buf.at[me],
                    buf.at[me],
                    send_sems.at[s],
                    recv_sems.at[s],
                    axis,
                    partner(me, s, count),
                )
            )
        return copies

    def arrive(copies):
        for copy in copies:
            copy.wait_recv()

    tok = gather(x_all, tok_send, tok_recv, "tp", me_tp, n_tp)

    loads["len"].wait()
    row_id = lax.broadcasted_iota(jnp.int32, (state_rows, chans), 0)
    live_len = jnp.zeros((state_rows, chans), jnp.int32)
    for r in range(state_rows):
        live_len = jnp.where(row_id == r, len_s[r], live_len)
    loads["decay"].wait()
    neg = -decay_v[...]
    rate = -8.0 * (jnp.maximum(neg, 0.0) + jnp.log1p(jnp.exp(-jnp.abs(neg))))
    loads["gain"].wait()
    gains = gain_v[...]

    arrive(tok)
    current = x_all[...].astype(jnp.float32).reshape(all_rows, width)

    def lane_squares(block):
        squares = None
        for c in range(0, width, LANES):
            piece = block[:, c : c + LANES]
            squares = piece * piece if squares is None else squares + piece * piece
        return squares

    def dot(a, b):
        return jnp.dot(a, b, preferred_element_type=jnp.float32)

    def push(l, steps, out, into, send_sems, recv_sems):
        copies = []
        for s in steps:
            target = partner(me_dp, s, n_dp)
            copies.append(
                send(
                    out.at[l, target],
                    into.at[l, s],
                    send_sems.at[l, s],
                    recv_sems.at[l, s],
                    "dp",
                    target,
                )
            )
        return copies

    group = rows // state_rows
    my_group = me_dp // group

    def steps_of(g):
        return [s for s in range(g * group, (g + 1) * group) if s]

    def project(l, block, steps, where):
        count = block.shape[0] // state_rows
        sq_out[l, where] = lane_squares(block).reshape(count, state_rows, LANES)
        copies = [push(l, steps, sq_out, sq_in, sq_send, sq_recv)]
        scaled = (block * gains[l : l + 1]).astype(jnp.bfloat16)
        if l == 0:
            loads["win"].wait()
        part = dot(scaled, win_v[l]).reshape(count, state_rows, chans)
        val_out[l, where] = part.astype(jnp.bfloat16)
        copies.append(push(l, steps, val_out, val_in, val_send, val_recv))
        if l == 0:
            loads["wgate"].wait()
        part = dot(scaled, wgate_v[l]).reshape(count, state_rows, chans)
        gate_out[l, where] = part.astype(jnp.bfloat16)
        copies.append(push(l, steps, gate_out, gate_in_buf, gate_send, gate_recv))
        return copies

    flying = project(0, current, order_of(n_dp), slice(None))
    late = []

    for l in range(layers):
        sq_copies, val_copies, gate_copies = flying
        if l == 0:
            for name in ("cw", "cs", "rs", "wrec", "winj"):
                loads[name].wait()
        conv_taps = cw_v[l].astype(jnp.float32)
        old = [cs_v[l, t].astype(jnp.float32) for t in range(taps)]
        history = jnp.zeros((state_rows, chans), jnp.float32)
        for back in range(1, taps + 1):
            history = history + conv_taps[taps - back : taps - back + 1] * jnp.where(
                back < live_len, old[taps - back], 0.0
            )
        previous = jnp.where(live_len > 1, rs_v[l], 0.0)
        for t in range(1, taps):
            new_conv[l, t - 1] = cs_v[l, t]

        arrive(sq_copies)
        total = sq_out[l, me_dp]
        for s in range(1, n_dp):
            total = total + sq_in[l, s]
        scale = lax.rsqrt(jnp.sum(total, axis=1, keepdims=True) / model + EPS)
        arrive(val_copies)
        value = val_out[l, me_dp].astype(jnp.float32)
        for s in range(1, n_dp):
            value = value + val_in[l, s].astype(jnp.float32)
        value = value * scale
        new_conv[l, taps - 1] = value.astype(jnp.bfloat16)
        conv_out = conv_taps[taps : taps + 1] * value + history
        conv_low = conv_out.astype(jnp.bfloat16)
        rec_parts = []
        inj_parts = []
        for b in range(blocks):
            piece = conv_low[:, b * blk : (b + 1) * blk]
            rec_parts.append(jnp.dot(piece, wrec_v[l, b], preferred_element_type=jnp.float32))
            inj_parts.append(jnp.dot(piece, winj_v[l, b], preferred_element_type=jnp.float32))
        rec_gate = jax.nn.sigmoid(jnp.concatenate(rec_parts, axis=1))
        inp_gate = jax.nn.sigmoid(jnp.concatenate(inj_parts, axis=1))
        log_decay = rate[l : l + 1] * rec_gate
        half = jnp.tanh(log_decay)
        hidden = jnp.exp(log_decay) * previous + jnp.sqrt(-2.0 * half / (1.0 - half)) * (
            inp_gate * conv_out
        )
        new_rec[l] = hidden
        arrive(gate_copies)
        gate = gate_out[l, me_dp].astype(jnp.float32)
        for s in range(1, n_dp):
            gate = gate + gate_in_buf[l, s].astype(jnp.float32)
        gate = gate * scale
        read_all[l, me_dp] = (hidden * jax.nn.gelu(gate)).astype(jnp.bfloat16)
        read_copies = dict(
            zip(
                order_of(n_dp),
                gather(read_all.at[l], read_send.at[l], read_recv.at[l], "dp", me_dp, n_dp),
            )
        )
        if l == 0:
            loads["wout"].wait()
        residual = x_all if l == 0 else x_keep.at[l - 1]
        parts = []
        for g in range(n_tp):
            owner = partner(my_group, g, n_tp)
            arrive([read_copies[s] for s in steps_of(g)])
            reads = read_all[l, pl.ds(owner * group, group)].astype(jnp.float32)
            reads = reads.reshape(rows, chans).astype(jnp.bfloat16)
            branch = dot(reads, wout_v[l]).astype(jnp.bfloat16)
            if l < layers - 1:
                mine = part_all.at[l, me_tp, owner]
                mine[...] = branch
                copies = []
                for s in order_of(n_tp):
                    copies.append(
                        send(
                            mine,
                            mine,
                            part_send.at[l, g, s],
                            part_recv.at[l, g, s],
                            "tp",
                            partner(me_tp, s, n_tp),
                        )
                    )
                parts.append(copies)
            else:
                last_out[owner] = branch
                copy = pltpu.make_async_remote_copy(
                    src_ref=last_out.at[owner],
                    dst_ref=last_in.at[me_tp],
                    send_sem=last_send.at[g],
                    recv_sem=last_recv.at[me_tp],
                    device_id={"tp": owner},
                    device_id_type=MESH,
                )
                late.append((owner, copy))
                pl.when(owner != me_tp)(copy.start)
        if l < layers - 1:
            flying = [[], [], []]
            for g in range(n_tp):
                owner = partner(my_group, g, n_tp)
                arrive(parts[g])
                block = residual[owner].astype(jnp.float32)
                for t in range(n_tp):
                    block = block + part_all[l, t, owner].astype(jnp.float32)
                block = block.astype(jnp.bfloat16)
                x_keep[l, owner] = block
                copies = project(
                    l + 1, block.astype(jnp.float32), steps_of(g), pl.ds(owner * group, group)
                )
                for kind, more in zip(flying, copies):
                    kind.extend(more)
        else:
            final = residual[me_tp].astype(jnp.float32) + last_out[me_tp].astype(jnp.float32)
            for s in range(1, n_tp):
                other = partner(me_tp, s, n_tp)
                pltpu.make_async_remote_copy(
                    src_ref=last_out.at[other],
                    dst_ref=last_in.at[other],
                    send_sem=last_send.at[s],
                    recv_sem=last_recv.at[other],
                    device_id={"tp": other},
                    device_id_type=MESH,
                ).wait_recv()
                final = final + last_in[other].astype(jnp.float32)
            mixed[...] = final.astype(jnp.bfloat16)
    for owner, copy in late:
        pl.when(owner != me_tp)(copy.wait_send)
    for copy in sent:
        copy.wait_send()


def flush(*refs):
    count = len(refs) // 2
    sems = refs[-1]
    copies = [
        pltpu.make_async_copy(src, dst, sems.at[i])
        for i, (src, dst) in enumerate(zip(refs[:count], refs[count : 2 * count]))
    ]
    for copy in copies:
        copy.start()
    for copy in copies:
        copy.wait()


def body(n_tp, n_dp, *args):
    (tokens, norm_gain, w_input, w_gate, w_recur, w_inject, conv_weight, decay_param, w_output,
     lengths, conv_state, rec_state) = args
    layers = w_input.shape[0]
    rows, width = tokens.shape
    state_rows = lengths.shape[0]
    chans = w_input.shape[2]
    all_rows = rows * n_tp
    bf16, f32 = jnp.bfloat16, jnp.float32
    like = lambda a: pltpu.VMEM(a.shape, a.dtype)
    dma = pltpu.SemaphoreType.DMA
    vmem = pl.BlockSpec(memory_space=pltpu.VMEM)
    shapes = ((tokens.shape, bf16), (conv_state.shape, bf16), (rec_state.shape, f32))
    held = pl.pallas_call(
        functools.partial(kernel, n_tp, n_dp),
        out_shape=tuple(pltpu.VMEM(*each) for each in shapes),
        in_specs=[pl.BlockSpec(memory_space=pl.ANY)] * len(args),
        out_specs=(vmem, vmem, vmem),
        scratch_shapes=[
            like(norm_gain),
            like(w_input),
            like(w_gate),
            like(w_recur),
            like(w_inject),
            like(conv_weight),
            like(decay_param),
            like(w_output),
            pltpu.SMEM(lengths.shape, lengths.dtype),
            like(conv_state),
            like(rec_state),
            pltpu.VMEM((n_tp, rows, width), bf16),
            pltpu.VMEM((layers, n_tp, rows, width), bf16),
            pltpu.VMEM((layers, n_dp, state_rows, LANES), f32),
            pltpu.VMEM((layers, n_dp, state_rows, LANES), f32),
            pltpu.VMEM((layers, n_dp, state_rows, chans), bf16),
            pltpu.VMEM((layers, n_dp, state_rows, chans), bf16),
            pltpu.VMEM((layers, n_dp, state_rows, chans), bf16),
            pltpu.VMEM((layers, n_dp, state_rows, chans), bf16),
            pltpu.VMEM((layers, n_dp, state_rows, chans), bf16),
            pltpu.VMEM((layers, n_tp, n_tp, rows, width), bf16),
            pltpu.VMEM((n_tp, rows, width), bf16),
            pltpu.VMEM((n_tp, rows, width), bf16),
            dma((12,)),
            dma((n_tp,)),
            dma((n_tp,)),
            dma((layers, n_dp)),
            dma((layers, n_dp)),
            dma((layers, n_dp)),
            dma((layers, n_dp)),
            dma((layers, n_dp)),
            dma((layers, n_dp)),
            dma((layers, n_dp)),
            dma((layers, n_dp)),
            dma((layers, n_tp, n_tp)),
            dma((layers, n_tp, n_tp)),
            dma((n_tp,)),
            dma((n_tp,)),
        ],
        compiler_params=pltpu.CompilerParams(collective_id=0, has_side_effects=True),
    )(*args)
    return pl.pallas_call(
        flush,
        out_shape=tuple(jax.ShapeDtypeStruct(*each) for each in shapes),
        in_specs=[vmem] * len(shapes),
        out_specs=tuple(pl.BlockSpec(memory_space=pl.ANY) for _ in shapes),
        scratch_shapes=[dma((len(shapes),))],
    )(*[pltpu.with_memory_space_constraint(each, pltpu.VMEM) for each in held])


def solution(mesh):
    n_tp, n_dp = mesh.shape["tp"], mesh.shape["dp"]
    placed = (
        P("tp", "dp"),
        P(None, "dp"),
        P(None, "dp", "tp"),
        P(None, "dp", "tp"),
        P(None, "tp", None, None),
        P(None, "tp", None, None),
        P(None, None, "tp"),
        P(None, "tp"),
        P(None, "tp", "dp"),
        P("dp"),
        P(None, None, "dp", "tp"),
        P(None, "dp", "tp"),
    )
    return jax.shard_map(
        functools.partial(body, n_tp, n_dp),
        mesh=mesh,
        in_specs=placed,
        out_specs=(P("tp", "dp"), P(None, None, "dp", "tp"), P(None, "dp", "tp")),
        check_vma=False,
    )
```
